32 devices in a mesh: rep: 2 (over x), fs: 4 (over z), tp: 4 (over y, core).
Axes of the slice: x: 2, y: 2, z: 4, core: 2. Of those that a mesh axis runs over, the one named last changes fastest.
Arguments:
- tokens: bfloat16 [3072, 2048], P(('rep', 'fs'), 'tp'), may hold values from -6 to 6
- norm_gain: bfloat16 [2048], replicated, may hold values from 0.099609375 to 1.8984375
- w_gate: bfloat16 [2048, 5120], P('fs', 'tp'), may hold values from -0.125 to 0.125
- w_up: bfloat16 [2048, 5120], P('fs', 'tp'), may hold values from -0.125 to 0.125
- w_down: bfloat16 [5120, 2048], P('tp', 'fs'), may hold values from -0.078125 to 0.078125
- cotangent: bfloat16 [3072, 2048], P(('rep', 'fs'), 'tp'), may hold values from -6 to 6
Outputs:
- grad_tokens: bfloat16 [3072, 2048], P(('rep', 'fs'), 'tp')
- grad_gain: float32 [2048], P('tp')
- grad_gate: float32 [2048, 5120], P('fs', 'tp')
- grad_up: float32 [2048, 5120], P('fs', 'tp')
- grad_down: float32 [5120, 2048], P('tp', 'fs')
- gate_up_sq: float32 [2, 2048], P(None, 'fs')
- down_sq: float32 [5120], P('tp')
The draws below stay inside these ranges and needn't reach their ends.
All inputs are finite; a program needn't handle non-finite values.
Results may differ from the reference program's by a relative error of at most 0.018.
Values may be sent and summed in bfloat16 or wider, within the bound.
A program may use at most 128 MiB of HBM per device.

```python
import jax
import jax.numpy as jnp
from jax import lax

D = 2048
FF = 5120
TOKENS = 3072


def raised(array, own_key, source, target, shards_of, factor):
    def block_of(position):
        return (jnp.arange(array.shape[position]) // (array.shape[position] // shards_of)).reshape((-1,) + (1,) * (array.ndim - 1 - position))

    first = jax.random.permutation(own_key, shards_of)[block_of(target)]
    far = (block_of(target) + shards_of // 2) % shards_of
    return jnp.where((block_of(source) == first) | (block_of(source) == far), factor * array, array)


def block_scale(rng, extent, pieces, smallest, top_value):
    factor_of = 1.0
    for position, shards_of in pieces:
        draws = jax.random.uniform(jax.random.fold_in(jax.random.fold_in(rng, 6), position), (shards_of,), jnp.float32, smallest / len(pieces), top_value / len(pieces))
        factor_of = factor_of * jnp.repeat(jnp.exp(draws), extent[position] // shards_of).reshape((-1,) + (1,) * (len(extent) - 1 - position))
    return factor_of


def scatter_about(stream_key, shape, scale, reach, split=(), held_as=jnp.bfloat16):
    gain = block_scale(stream_key, shape, split, -0.22, 0.18) if split else 1.0
    drawn = jax.random.normal(stream_key, shape, jnp.float32) * scale * gain
    return jnp.minimum(jnp.maximum(drawn, -reach), reach).astype(held_as)


def heavy_noise(own_key, extent, scale, limit, split, heavy, held_as=jnp.bfloat16):
    entries = scale * jax.random.normal(own_key, extent, jnp.float32)
    if split:
        entries = entries * block_scale(own_key, extent, split, -0.22, 0.18)
    return jnp.clip(raised(entries, jax.random.fold_in(own_key, 3), *heavy), -limit, limit).astype(held_as)


def setup_inputs(seed: int = 0) -> dict:
    splits = jax.random.split(jax.random.key(seed), 7)
    tokens = scatter_about(splits[0], (TOKENS, D), 1.0, 6.0, ((0, 8), (1, 4)))
    norm_gain = jnp.clip(1.0 + 0.18 * jax.random.normal(splits[1], (D,), jnp.float32), 0.099609375, 1.8984375).astype(jnp.bfloat16)
    w_gate = scatter_about(splits[2], (D, FF), D ** -0.5, 0.125, ((0, 4), (1, 4)))
    w_up = scatter_about(splits[3], (D, FF), D ** -0.5, 0.125, ((0, 4), (1, 4)))
    w_down = scatter_about(splits[4], (FF, D), FF ** -0.5, 0.078125, ((0, 4), (1, 4)))
    cotangent = heavy_noise(splits[5], (TOKENS, D), 1.0, 6.0, ((0, 8), (1, 4)), (0, 1, 8, 2.0))
    return {"tokens": tokens, "norm_gain": norm_gain, "w_gate": w_gate, "w_up": w_up, "w_down": w_down, "cotangent": cotangent}


def reference(tokens, norm_gain, w_gate, w_up, w_down, cotangent):
    wide_tokens = tokens.astype(jnp.float32)
    gain_f = norm_gain.astype(jnp.float32)
    inverse = jax.lax.rsqrt(lax.optimization_barrier(jnp.mean(wide_tokens * wide_tokens, axis=-1, keepdims=True)) + 1e-06)
    normed = (wide_tokens * inverse * gain_f).astype(jnp.bfloat16)
    gate = jnp.dot(normed, w_gate, preferred_element_type=jnp.float32)
    up_proj = jnp.dot(normed, w_up, preferred_element_type=jnp.float32)
    sigma = jax.nn.sigmoid(gate)
    active = gate * sigma
    hidden = (active * up_proj).astype(jnp.bfloat16)
    back = 0.5 * jnp.dot(cotangent, w_down.T, preferred_element_type=jnp.float32)
    d_up = (back * active).astype(jnp.bfloat16)
    d_gate = (back * up_proj * sigma * (1.0 + gate * (1.0 - sigma))).astype(jnp.bfloat16)
    d_normed = jnp.dot(d_gate, w_gate.T, preferred_element_type=jnp.float32) + jnp.dot(d_up, w_up.T, preferred_element_type=jnp.float32)
    grad_gain = lax.optimization_barrier(jnp.sum(d_normed * wide_tokens * inverse, axis=0))
    scaled_grad = d_normed * gain_f
    rowdot = lax.optimization_barrier(jnp.sum(scaled_grad * wide_tokens, axis=-1, keepdims=True))
    grad_tokens = (cotangent.astype(jnp.float32) + inverse * scaled_grad - wide_tokens * inverse ** 3 * rowdot / D).astype(jnp.bfloat16)
    grad_gate = jnp.einsum('td,tf->df', normed, d_gate, preferred_element_type=jnp.float32)
    grad_up = jnp.einsum('td,tf->df', normed, d_up, preferred_element_type=jnp.float32)
    grad_down = 0.5 * jnp.einsum('tf,td->fd', hidden, cotangent, preferred_element_type=jnp.float32)
    gate_up_sq = jnp.stack([lax.optimization_barrier(jnp.sum(grad_gate * grad_gate, axis=1)), lax.optimization_barrier(jnp.sum(grad_up * grad_up, axis=1))])
    down_sq = lax.optimization_barrier(jnp.sum(grad_down * grad_down, axis=1))
    return (grad_tokens, grad_gain, grad_gate, grad_up, grad_down, gate_up_sq, down_sq)
```

```python
import functools

import jax
import jax.numpy as jnp
from jax import lax
from jax.experimental import pallas as pl
from jax.experimental.pallas import tpu as pltpu
from jax.sharding import PartitionSpec as P

MESH = pl.DeviceIdType.MESH


def contract_last(left, right):
    return lax.dot_general(
        left, right, (((1,), (1,)), ((), ())), preferred_element_type=jnp.float32
    )


def contract_first(left, right):
    return lax.dot_general(
        left, right, (((0,), (0,)), ((), ())), preferred_element_type=jnp.float32
    )


def send(source, target, send_sem, recv_sem, where):
    copy = pltpu.make_async_remote_copy(
        src_ref=source,
        dst_ref=target,
        send_sem=send_sem,
        recv_sem=recv_sem,
        device_id=where,
        device_id_type=MESH,
    )
    copy.start()
    return copy


def greet(peers):
    barrier = pltpu.get_barrier_semaphore()
    for peer in peers:
        pl.semaphore_signal(barrier, inc=1, device_id=peer, device_id_type=MESH)
    pl.semaphore_wait(barrier, len(peers))


def keep_own(sources, holders, targets, sems):
    count = len(sources)
    loads = [
        pltpu.make_async_copy(sources[i], holders[i], sems.at[0, i]) for i in range(count)
    ]
    stores = [
        pltpu.make_async_copy(holders[i], targets[i], sems.at[1, i]) for i in range(count)
    ]
    for load in loads:
        load.start()

    def finish():
        for load, store in zip(loads, stores):
            load.wait()
            store.start()
        for store in stores:
            store.wait()

    return finish


def weights_kernel(n_fs, n_tp, *refs):
    tokens, cot, w_gate, w_up, w_down = refs[:5]
    whole_x, whole_dy, full_gate, full_up, full_down = refs[5:10]
    holders = refs[10:15]
    own_sem, ring_send, ring_recv, rep_send, rep_recv, tp_send, tp_recv = refs[15:]
    r, z, t = lax.axis_index("rep"), lax.axis_index("fs"), lax.axis_index("tp")
    right, left = lax.rem(z + 1, n_fs), lax.rem(z + n_fs - 1, n_fs)
    partner = {"rep": 1 - r}
    sources = (w_gate, w_up, w_down)
    targets = (full_gate, full_up, full_down)
    rows = w_gate.shape[0]
    hidden = w_down.shape[0]
    local = tokens.shape[1]
    reach = n_fs // 2

    def own_piece(m, half):
        size = (hidden if m == 2 else rows) // 2
        return sources[m].at[pl.ds(pl.multiple_of(half * size, size), size), :]

    def piece(m, owner, half):
        if m == 2:
            size = hidden // 2
            return targets[m].at[
                pl.ds(pl.multiple_of(half * size, size), size),
                pl.ds(pl.multiple_of(owner * rows, rows), rows),
            ]
        size = rows // 2
        return targets[m].at[
            pl.ds(pl.multiple_of(owner * rows + half * size, size), size), :
        ]

    peers = [{"fs": right}, {"fs": left}, partner]
    peers += [{"tp": lax.rem(t + j, n_tp)} for j in range(1, n_tp)]
    greet(peers)

    ends = []

    def hop(m, side, d):
        half = r if side == 0 else 1 - r
        owner = lax.rem(z + (n_fs - (d - 1) if side == 0 else d - 1), n_fs)
        place = piece(m, owner, half)
        return send(
            own_piece(m, half) if d == 1 else place,
            place,
            ring_send.at[m, side, d - 1],
            ring_recv.at[m, side, d - 1],
            {"fs": right if side == 0 else left},
        )

    flying = {}
    for m in range(3):
        for side in range(2):
            flying[m, side] = hop(m, side, 1)
    for a, (source, target) in enumerate(((tokens, whole_x), (cot, whole_dy))):
        place = target.at[:, pl.ds(pl.multiple_of(t * local, local), local)]
        for j in range(1, n_tp):
            ends.append(
                send(
                    source,
                    place,
                    tp_send.at[a, j - 1],
                    tp_recv.at[a, j - 1],
                    {"tp": lax.rem(t + j, n_tp)},
                )
            )
    mine = pl.ds(pl.multiple_of(t * local, local), local)
    band = pl.ds(pl.multiple_of(z * rows, rows), rows)
    finish = keep_own(
        (tokens, cot, w_gate, w_up, w_down),
        holders,
        (
            whole_x.at[:, mine],
            whole_dy.at[:, mine],
            full_gate.at[band, :],
            full_up.at[band, :],
            full_down.at[:, band],
        ),
        own_sem,
    )
    finish()
    for d in range(1, reach + 1):
        for m in range(3):
            for side in range(2):
                copy = flying[m, side]
                copy.wait_recv()
                if d < reach:
                    flying[m, side] = hop(m, side, d + 1)
                    half = r if side == 0 else 1 - r
                    owner = lax.rem(z + (n_fs - d if side == 0 else d), n_fs)
                    place = piece(m, owner, half)
                    ends.append(
                        send(
                            place,
                            place,
                            rep_send.at[m, side, d - 1],
                            rep_recv.at[m, side, d - 1],
                            partner,
                        )
                    )
                copy.wait_send()
    for copy in ends:
        copy.wait()


def gather_weights(n_fs, n_tp, tokens, cot, w_gate, w_up, w_down):
    count, local = tokens.shape
    rows, hidden = w_gate.shape
    width = rows * n_fs
    dtype = tokens.dtype
    shapes = [
        (count, width),
        (count, width),
        (width, hidden),
        (width, hidden),
        (hidden, width),
    ]
    held = (tokens, cot, w_gate, w_up, w_down)
    reach = n_fs // 2
    moved = sum(2 * a * b for a, b in shapes)
    dma = pltpu.SemaphoreType.DMA
    return pl.pallas_call(
        functools.partial(weights_kernel, n_fs, n_tp),
        out_shape=[jax.ShapeDtypeStruct(s, dtype) for s in shapes],
        in_specs=[pl.BlockSpec(memory_space=pl.ANY)] * 5,
        out_specs=[pl.BlockSpec(memory_space=pl.ANY)] * 5,
        scratch_shapes=[pltpu.VMEM(a.shape, a.dtype) for a in held]
        + [
            dma((2, 5)),
            dma((3, 2, reach)),
            dma((3, 2, reach)),
            dma((3, 2, max(reach - 1, 1))),
            dma((3, 2, max(reach - 1, 1))),
            dma((2, n_tp - 1)),
            dma((2, n_tp - 1)),
        ],
        compiler_params=pltpu.CompilerParams(collective_id=0, has_side_effects=True),
        cost_estimate=pl.CostEstimate(flops=0, bytes_accessed=16 * moved, transcendentals=0),
        name="gather_weights",
    )(*held)


def tokens_kernel(n_fs, n_act, n_swap, *refs):
    total = n_act + n_swap
    acts, swaps = refs[:n_act], refs[n_act:total]
    act_outs, swap_outs = refs[total : total + n_act], refs[total + n_act : 2 * total]
    holders = refs[2 * total : 3 * total]
    own_sem, ring_send, ring_recv, swap_send, swap_recv = refs[3 * total :]
    z = lax.axis_index("fs")
    right, left = lax.rem(z + 1, n_fs), lax.rem(z + n_fs - 1, n_fs)
    count = acts[0].shape[0]
    reach = n_fs // 2
    greet([{"fs": lax.rem(z + j, n_fs)} for j in range(1, n_fs)])

    def hop(m, side, d):
        owner = lax.rem(z + (n_fs - (d - 1) if side == 0 else d - 1), n_fs)
        first, size = 0, count
        if d == reach:
            size = count // 2
            first = side * size
        place = act_outs[m].at[pl.ds(pl.multiple_of(owner * count + first, size), size), :]
        source = acts[m].at[pl.ds(first, size), :] if d == 1 else place
        return send(
            source,
            place,
            ring_send.at[m, side, d - 1],
            ring_recv.at[m, side, d - 1],
            {"fs": right if side == 0 else left},
        )

    ends = []
    flying = {}
    band = pl.ds(pl.multiple_of(z * count, count), count)
    for m in range(n_act):
        for side in range(2):
            flying[m, side] = hop(m, side, 1)
    for a in range(n_swap):
        cut = swap_outs[a].shape[1]
        for j in range(1, n_fs):
            peer = lax.rem(z + j, n_fs)
            ends.append(
                send(
                    swaps[a].at[:, pl.ds(pl.multiple_of(peer * cut, cut), cut)],
                    swap_outs[a].at[band, :],
                    swap_send.at[a, j - 1],
                    swap_recv.at[a, j - 1],
                    {"fs": peer},
                )
            )
    sources = list(acts)
    for a in range(n_swap):
        cut = swap_outs[a].shape[1]
        sources.append(swaps[a].at[:, pl.ds(pl.multiple_of(z * cut, cut), cut)])
    finish = keep_own(
        sources, holders, [out.at[band, :] for out in act_outs + swap_outs], own_sem
    )
    finish()
    for d in range(1, reach + 1):
        for m in range(n_act):
            for side in range(2):
                copy = flying[m, side]
                copy.wait_recv()
                if d < reach:
                    flying[m, side] = hop(m, side, d + 1)
                copy.wait_send()
    for copy in ends:
        copy.wait()


def gather_tokens(n_fs, collective_id, acts, swaps):
    count = acts[0].shape[0]
    outs = [jax.ShapeDtypeStruct((n_fs * count, a.shape[1]), a.dtype) for a in acts]
    outs += [jax.ShapeDtypeStruct((n_fs * count, a.shape[1] // n_fs), a.dtype) for a in swaps]
    reach = n_fs // 2
    dma = pltpu.SemaphoreType.DMA
    total = len(outs)
    n_swap = max(len(swaps), 1)
    moved = sum(2 * o.shape[0] * o.shape[1] for o in outs)
    return pl.pallas_call(
        functools.partial(tokens_kernel, n_fs, len(acts), len(swaps)),
        out_shape=outs,
        in_specs=[pl.BlockSpec(memory_space=pl.ANY)] * total,
        out_specs=[pl.BlockSpec(memory_space=pl.ANY)] * total,
        scratch_shapes=[pltpu.VMEM((count, o.shape[1]), o.dtype) for o in outs]
        + [
            dma((2, total)),
            dma((len(acts), 2, reach)),
            dma((len(acts), 2, reach)),
            dma((n_swap, n_fs - 1)),
            dma((n_swap, n_fs - 1)),
        ],
        compiler_params=pltpu.CompilerParams(
            collective_id=collective_id, has_side_effects=True
        ),
        cost_estimate=pl.CostEstimate(flops=0, bytes_accessed=16 * moved, transcendentals=0),
        name=f"gather_tokens_{collective_id}",
    )(*acts, *swaps)


def over_rep(part):
    part = part.astype(jnp.bfloat16)
    n_rep = lax.axis_size("rep")
    other = lax.ppermute(part, "rep", [(i, (i + 1) % n_rep) for i in range(n_rep)])
    return part, other


def added(pair):
    return pair[0].astype(jnp.float32) + pair[1].astype(jnp.float32)


def on_device(tokens, norm_gain, w_gate, w_up, w_down, cotangent):
    n_fs, n_tp = lax.axis_size("fs"), lax.axis_size("tp")
    whole_x, whole_dy, full_gate, full_up, full_down = gather_weights(
        n_fs, n_tp, tokens, cotangent, w_gate, w_up, w_down
    )
    width = whole_x.shape[1]
    wide_tokens = whole_x.astype(jnp.float32)
    gain_f = norm_gain.astype(jnp.float32)
    inverse = lax.rsqrt(jnp.mean(wide_tokens * wide_tokens, axis=-1, keepdims=True) + 1e-06)
    normed = (wide_tokens * inverse * gain_f).astype(jnp.bfloat16)
    gate = jnp.dot(normed, full_gate, preferred_element_type=jnp.float32)
    up_proj = jnp.dot(normed, full_up, preferred_element_type=jnp.float32)
    sigma = jax.nn.sigmoid(gate)
    active = gate * sigma
    hidden = (active * up_proj).astype(jnp.bfloat16)
    back = 0.5 * contract_last(whole_dy, full_down)
    d_up = (back * active).astype(jnp.bfloat16)
    d_gate = (back * up_proj * sigma * (1.0 + gate * (1.0 - sigma))).astype(jnp.bfloat16)

    all_hidden, rows_dy = gather_tokens(n_fs, 1, [hidden], [whole_dy])
    down_pair = over_rep(0.5 * contract_first(all_hidden, rows_dy))

    partial_normed = contract_last(d_gate, full_gate) + contract_last(d_up, full_up)
    d_normed = lax.psum_scatter(
        partial_normed.astype(jnp.bfloat16), "tp", scatter_dimension=1, tiled=True
    ).astype(jnp.float32)

    all_gate, rows_normed = gather_tokens(n_fs, 2, [d_gate], [normed])
    gate_pair = over_rep(contract_first(rows_normed, all_gate))
    (all_up,) = gather_tokens(n_fs, 3, [d_up], [])
    up_pair = over_rep(contract_first(rows_normed, all_up))

    local_width = d_normed.shape[1]
    local_gain = lax.dynamic_slice_in_dim(
        gain_f, lax.axis_index("tp") * local_width, local_width, 0
    )
    local_tokens = tokens.astype(jnp.float32)
    scaled_grad = d_normed * local_gain
    rowdot = lax.psum(jnp.sum(scaled_grad * local_tokens, axis=-1), "tp")
    grad_tokens = (
        cotangent.astype(jnp.float32)
        + inverse * scaled_grad
        - local_tokens * inverse**3 * rowdot[:, None] / width
    ).astype(jnp.bfloat16)
    grad_gain = lax.psum(jnp.sum(d_normed * local_tokens * inverse, axis=0), ("rep", "fs"))

    grad_down = added(down_pair)
    down_sq = lax.psum(jnp.sum(grad_down * grad_down, axis=1), "fs")
    grad_gate = added(gate_pair)
    grad_up = added(up_pair)
    gate_up_sq = lax.psum(
        jnp.stack([jnp.sum(grad_gate * grad_gate, axis=1), jnp.sum(grad_up * grad_up, axis=1)]),
        "tp",
    )
    return (grad_tokens, grad_gain, grad_gate, grad_up, grad_down, gate_up_sq, down_sq)


def solution(mesh):
    placed = (
        P(("rep", "fs"), "tp"),
        P(),
        P("fs", "tp"),
        P("fs", "tp"),
        P("tp", "fs"),
        P(("rep", "fs"), "tp"),
    )
    return jax.shard_map(
        on_device,
        mesh=mesh,
        in_specs=placed,
        out_specs=(
            P(("rep", "fs"), "tp"),
            P("tp"),
            P("fs", "tp"),
            P("fs", "tp"),
            P("tp", "fs"),
            P(None, "fs"),
            P("tp"),
        ),
        check_vma=False,
    )
```

```python
import functools

import jax
import jax.numpy as jnp
from jax import lax
from jax.experimental import pallas as pl
from jax.experimental.pallas import tpu as pltpu
from jax.sharding import PartitionSpec as P

MESH = pl.DeviceIdType.MESH


def contract_last(left, right):
    return lax.dot_general(
        left, right, (((1,), (1,)), ((), ())), preferred_element_type=jnp.float32
    )


def contract_first(left, right):
    return lax.dot_general(
        left, right, (((0,), (0,)), ((), ())), preferred_element_type=jnp.float32
    )


def remote(source, target, send_sem, recv_sem, where):
    return pltpu.make_async_remote_copy(
        src_ref=source,
        dst_ref=target,
        send_sem=send_sem,
        recv_sem=recv_sem,
        device_id=where,
        device_id_type=MESH,
    )


def line_sends(z, n_fs, side, d):
    if side == 0:
        return jnp.logical_and(z >= d - 1, z <= n_fs - 2)
    return jnp.logical_and(z + d <= n_fs, z >= 1)


def line_receives(z, n_fs, side, d):
    return z >= d if side == 0 else z + d <= n_fs - 1


def greet(peers):
    barrier = pltpu.get_barrier_semaphore()
    for peer in peers:
        pl.semaphore_signal(barrier, inc=1, device_id=peer, device_id_type=MESH)
    pl.semaphore_wait(barrier, len(peers))


def keep_own(sources, holders, targets, sems):
    count = len(sources)
    loads = [
        pltpu.make_async_copy(sources[i], holders[i], sems.at[0, i]) for i in range(count)
    ]
    stores = [
        pltpu.make_async_copy(holders[i], targets[i], sems.at[1, i]) for i in range(count)
    ]
    for load in loads:
        load.start()

    def finish():
        for load, store in zip(loads, stores):
            load.wait()
            store.start()
        for store in stores:
            store.wait()

    return finish


def weights_kernel(n_fs, n_tp, *refs):
    tokens, cot, w_gate, w_up, w_down = refs[:5]
    whole_x, whole_dy, full_gate, full_up, full_down = refs[5:10]
    holders = refs[10:15]
    own_sem, ring_send, ring_recv, rep_send, rep_recv, tp_send, tp_recv = refs[15:]
    r, z, t = lax.axis_index("rep"), lax.axis_index("fs"), lax.axis_index("tp")
    right, left = lax.rem(z + 1, n_fs), lax.rem(z + n_fs - 1, n_fs)
    partner = {"rep": 1 - r}
    sources = (w_gate, w_up, w_down)
    targets = (full_gate, full_up, full_down)
    rows = w_gate.shape[0]
    hidden = w_down.shape[0]
    local = tokens.shape[1]

    def own_piece(m, half):
        size = (hidden if m == 2 else rows) // 2
        return sources[m].at[pl.ds(pl.multiple_of(half * size, size), size), :]

    def piece(m, owner, half):
        if m == 2:
            size = hidden // 2
            return targets[m].at[
                pl.ds(pl.multiple_of(half * size, size), size),
                pl.ds(pl.multiple_of(owner * rows, rows), rows),
            ]
        size = rows // 2
        return targets[m].at[
            pl.ds(pl.multiple_of(owner * rows + half * size, size), size), :
        ]

    peers = [{"fs": right}, {"fs": left}, partner]
    peers += [{"tp": lax.rem(t + j, n_tp)} for j in range(1, n_tp)]
    greet(peers)

    def owner_of(side, back):
        return lax.rem(z + (n_fs - back if side == 0 else back), n_fs)

    def hop(m, side, d):
        place = piece(m, owner_of(side, d - 1), r)
        return remote(
            own_piece(m, r) if d == 1 else place,
            place,
            ring_send.at[m, side, d - 1],
            ring_recv.at[m, side, d - 1],
            {"fs": right if side == 0 else left},
        )

    def arrival(m, side, d):
        place = piece(m, owner_of(side, d), r)
        return remote(
            place,
            place,
            ring_send.at[m, side, d - 1],
            ring_recv.at[m, side, d - 1],
            {"fs": right if side == 0 else left},
        )

    def across(m, side, d):
        place = piece(m, owner_of(side, d), r)
        return remote(
            place, place, rep_send.at[m, side, d - 1], rep_recv.at[m, side, d - 1], partner
        )

    for m in range(3):
        for side in range(2):

            @pl.when(line_sends(z, n_fs, side, 1))
            def _():
                hop(m, side, 1).start()

    ends = []
    for a, (source, target) in enumerate(((tokens, whole_x), (cot, whole_dy))):
        place = target.at[:, pl.ds(pl.multiple_of(t * local, local), local)]
        for j in range(1, n_tp):
            copy = remote(
                source,
                place,
                tp_send.at[a, j - 1],
                tp_recv.at[a, j - 1],
                {"tp": lax.rem(t + j, n_tp)},
            )
            copy.start()
            ends.append(copy)
    mine = pl.ds(pl.multiple_of(t * local, local), local)
    band = pl.ds(pl.multiple_of(z * rows, rows), rows)
    finish = keep_own(
        (tokens, cot, w_gate, w_up, w_down),
        holders,
        (
            whole_x.at[:, mine],
            whole_dy.at[:, mine],
            full_gate.at[band, :],
            full_up.at[band, :],
            full_down.at[:, band],
        ),
        own_sem,
    )
    finish()
    for d in range(1, n_fs):
        for m in range(3):
            for side in range(2):

                @pl.when(line_receives(z, n_fs, side, d))
                def _():
                    arrival(m, side, d).wait_recv()
                    if d < n_fs - 1:

                        @pl.when(line_sends(z, n_fs, side, d + 1))
                        def _():
                            hop(m, side, d + 1).start()

                    across(m, side, d).start()

    for d in range(1, n_fs):
        for m in range(3):
            for side in range(2):

                @pl.when(line_sends(z, n_fs, side, d))
                def _():
                    hop(m, side, d).wait_send()

                @pl.when(line_receives(z, n_fs, side, d))
                def _():
                    across(m, side, d).wait()

    for copy in ends:
        copy.wait()


def gather_weights(n_fs, n_tp, tokens, cot, w_gate, w_up, w_down):
    count, local = tokens.shape
    rows, hidden = w_gate.shape
    width = rows * n_fs
    dtype = tokens.dtype
    shapes = [
        (count, width),
        (count, width),
        (width, hidden),
        (width, hidden),
        (hidden, width),
    ]
    held = (tokens, cot, w_gate, w_up, w_down)
    moved = sum(2 * a * b for a, b in shapes)
    dma = pltpu.SemaphoreType.DMA
    return pl.pallas_call(
        functools.partial(weights_kernel, n_fs, n_tp),
        out_shape=[jax.ShapeDtypeStruct(s, dtype) for s in shapes],
        in_specs=[pl.BlockSpec(memory_space=pl.ANY)] * 5,
        out_specs=[pl.BlockSpec(memory_space=pl.ANY)] * 5,
        scratch_shapes=[pltpu.VMEM(a.shape, a.dtype) for a in held]
        + [
            dma((2, 5)),
            dma((3, 2, n_fs - 1)),
            dma((3, 2, n_fs - 1)),
            dma((3, 2, n_fs - 1)),
            dma((3, 2, n_fs - 1)),
            dma((2, n_tp - 1)),
            dma((2, n_tp - 1)),
        ],
        compiler_params=pltpu.CompilerParams(collective_id=0, has_side_effects=True),
        cost_estimate=pl.CostEstimate(flops=0, bytes_accessed=16 * moved, transcendentals=0),
        name="gather_weights",
    )(*held)


def tokens_kernel(n_fs, n_tp, n_act, n_swap, *refs):
    total = n_act + n_swap
    acts, swaps = refs[:n_act], refs[n_act:total]
    act_outs, swap_outs = refs[total : total + n_act], refs[total + n_act : 2 * total]
    holders = refs[2 * total : 3 * total]
    own_sem, ring_send, ring_recv = refs[3 * total : 3 * total + 3]
    swap_send, swap_recv, relay_send, relay_recv = refs[3 * total + 3 :]
    z, t = lax.axis_index("fs"), lax.axis_index("tp")
    right, left = lax.rem(z + 1, n_fs), lax.rem(z + n_fs - 1, n_fs)
    count = acts[0].shape[0]
    peers = [{"fs": lax.rem(z + j, n_fs)} for j in range(1, n_fs)]
    if n_swap:
        peers += [{"tp": lax.rem(t + j, n_tp)} for j in range(1, n_tp)]
    greet(peers)

    def rows_of(owner):
        return pl.ds(pl.multiple_of(owner * count, count), count)

    def owner_of(side, back):
        return lax.rem(z + (n_fs - back if side == 0 else back), n_fs)

    def hop(m, side, d):
        place = act_outs[m].at[rows_of(owner_of(side, d - 1)), :]
        return remote(
            acts[m] if d == 1 else place,
            place,
            ring_send.at[m, side, d - 1],
            ring_recv.at[m, side, d - 1],
            {"fs": right if side == 0 else left},
        )

    def arrival(m, side, d):
        place = act_outs[m].at[rows_of(owner_of(side, d)), :]
        return remote(
            place,
            place,
            ring_send.at[m, side, d - 1],
            ring_recv.at[m, side, d - 1],
            {"fs": right if side == 0 else left},
        )

    def swap(a, j):
        peer = lax.rem(z + j, n_fs)
        cut = swap_outs[a].shape[1]
        return remote(
            swaps[a].at[:, pl.ds(pl.multiple_of(peer * cut, cut), cut)],
            swap_outs[a].at[rows_of(z), :],
            swap_send.at[a, j - 1],
            swap_recv.at[a, j - 1],
            {"fs": peer},
        )

    def swapped(a, j):
        place = swap_outs[a].at[rows_of(owner_of(0, j)), :]
        return remote(
            place,
            place,
            swap_send.at[a, j - 1],
            swap_recv.at[a, j - 1],
            {"fs": lax.rem(z + j, n_fs)},
        )

    def relay(a, j, k):
        place = swap_outs[a].at[rows_of(owner_of(0, j)), :]
        return remote(
            place,
            place,
            relay_send.at[a, j - 1, k - 1],
            relay_recv.at[a, j - 1],
            {"tp": lax.rem(t + k, n_tp)},
        )

    hub = lax.rem(z, n_tp) == t

    def feeds(j):
        return lax.rem(lax.rem(z + j, n_fs), n_tp) == t

    for a in range(n_swap):
        for j in range(1, n_fs):

            @pl.when(feeds(j))
            def _():
                swap(a, j).start()

    for m in range(n_act):
        for side in range(2):

            @pl.when(line_sends(z, n_fs, side, 1))
            def _():
                hop(m, side, 1).start()

    sources = list(acts)
    for a in range(n_swap):
        cut = swap_outs[a].shape[1]
        sources.append(swaps[a].at[:, pl.ds(pl.multiple_of(z * cut, cut), cut)])
    finish = keep_own(
        sources, holders, [out.at[rows_of(z), :] for out in act_outs + swap_outs], own_sem
    )
    finish()
    if n_swap:

        @pl.when(hub)
        def _():
            for a in range(n_swap):
                for j in range(1, n_fs):
                    swapped(a, j).wait_recv()
                    for k in range(1, n_tp):
                        relay(a, j, k).start()

    for d in range(1, n_fs):
        for m in range(n_act):
            for side in range(2):

                @pl.when(line_receives(z, n_fs, side, d))
                def _():
                    arrival(m, side, d).wait_recv()
                    if d < n_fs - 1:

                        @pl.when(line_sends(z, n_fs, side, d + 1))
                        def _():
                            hop(m, side, d + 1).start()

    for d in range(1, n_fs):
        for m in range(n_act):
            for side in range(2):

                @pl.when(line_sends(z, n_fs, side, d))
                def _():
                    hop(m, side, d).wait_send()

    for a in range(n_swap):
        for j in range(1, n_fs):

            @pl.when(feeds(j))
            def _():
                swap(a, j).wait_send()

            @pl.when(hub)
            def _():
                for k in range(1, n_tp):
                    relay(a, j, k).wait_send()

            @pl.when(jnp.logical_not(hub))
            def _():
                relay(a, j, 1).wait_recv()


def gather_tokens(n_fs, n_tp, collective_id, acts, swaps):
    count = acts[0].shape[0]
    outs = [jax.ShapeDtypeStruct((n_fs * count, a.shape[1]), a.dtype) for a in acts]
    outs += [jax.ShapeDtypeStruct((n_fs * count, a.shape[1] // n_fs), a.dtype) for a in swaps]
    dma = pltpu.SemaphoreType.DMA
    total = len(outs)
    n_swap = max(len(swaps), 1)
    moved = sum(2 * o.shape[0] * o.shape[1] for o in outs)
    return pl.pallas_call(
        functools.partial(tokens_kernel, n_fs, n_tp, len(acts), len(swaps)),
        out_shape=outs,
        in_specs=[pl.BlockSpec(memory_space=pl.ANY)] * total,
        out_specs=[pl.BlockSpec(memory_space=pl.ANY)] * total,
        scratch_shapes=[pltpu.VMEM((count, o.shape[1]), o.dtype) for o in outs]
        + [
            dma((2, total)),
            dma((len(acts), 2, n_fs - 1)),
            dma((len(acts), 2, n_fs - 1)),
            dma((n_swap, n_fs - 1)),
            dma((n_swap, n_fs - 1)),
            dma((n_swap, n_fs - 1, n_tp - 1)),
            dma((n_swap, n_fs - 1)),
        ],
        compiler_params=pltpu.CompilerParams(
            collective_id=collective_id, has_side_effects=True
        ),
        cost_estimate=pl.CostEstimate(flops=0, bytes_accessed=16 * moved, transcendentals=0),
        name=f"gather_tokens_{collective_id}",
    )(*acts, *swaps)


def over_rep(part):
    part = part.astype(jnp.bfloat16)
    n_rep = lax.axis_size("rep")
    other = lax.ppermute(part, "rep", [(i, (i + 1) % n_rep) for i in range(n_rep)])
    return part, other


def added(pair):
    return pair[0].astype(jnp.float32) + pair[1].astype(jnp.float32)


def on_device(tokens, norm_gain, w_gate, w_up, w_down, cotangent):
    n_fs, n_tp = lax.axis_size("fs"), lax.axis_size("tp")
    whole_x, whole_dy, full_gate, full_up, full_down = gather_weights(
        n_fs, n_tp, tokens, cotangent, w_gate, w_up, w_down
    )
    width = whole_x.shape[1]
    wide_tokens = whole_x.astype(jnp.float32)
    gain_f = norm_gain.astype(jnp.float32)
    inverse = lax.rsqrt(jnp.mean(wide_tokens * wide_tokens, axis=-1, keepdims=True) + 1e-06)
    normed = (wide_tokens * inverse * gain_f).astype(jnp.bfloat16)
    gate = jnp.dot(normed, full_gate, preferred_element_type=jnp.float32)
    up_proj = jnp.dot(normed, full_up, preferred_element_type=jnp.float32)
    sigma = jax.nn.sigmoid(gate)
    active = gate * sigma
    hidden = (active * up_proj).astype(jnp.bfloat16)
    back = 0.5 * contract_last(whole_dy, full_down)
    d_up = (back * active).astype(jnp.bfloat16)
    d_gate = (back * up_proj * sigma * (1.0 + gate * (1.0 - sigma))).astype(jnp.bfloat16)

    all_hidden, rows_dy = gather_tokens(n_fs, n_tp, 1, [hidden], [whole_dy])
    down_pair = over_rep(0.5 * contract_first(all_hidden, rows_dy))

    partial_normed = contract_last(d_gate, full_gate) + contract_last(d_up, full_up)
    d_normed = lax.psum_scatter(
        partial_normed.astype(jnp.bfloat16), "tp", scatter_dimension=1, tiled=True
    ).astype(jnp.float32)

    all_gate, rows_normed = gather_tokens(n_fs, n_tp, 2, [d_gate], [normed])
    gate_pair = over_rep(contract_first(rows_normed, all_gate))
    (all_up,) = gather_tokens(n_fs, n_tp, 3, [d_up], [])
    up_pair = over_rep(contract_first(rows_normed, all_up))

    local_width = d_normed.shape[1]
    local_gain = lax.dynamic_slice_in_dim(
        gain_f, lax.axis_index("tp") * local_width, local_width, 0
    )
    local_tokens = tokens.astype(jnp.float32)
    scaled_grad = d_normed * local_gain
    rowdot = lax.psum(jnp.sum(scaled_grad * local_tokens, axis=-1), "tp")
    grad_tokens = (
        cotangent.astype(jnp.float32)
        + inverse * scaled_grad
        - local_tokens * inverse**3 * rowdot[:, None] / width
    ).astype(jnp.bfloat16)
    grad_gain = lax.psum(jnp.sum(d_normed * local_tokens * inverse, axis=0), ("rep", "fs"))

    grad_down = added(down_pair)
    down_sq = lax.psum(jnp.sum(grad_down * grad_down, axis=1), "fs")
    grad_gate = added(gate_pair)
    grad_up = added(up_pair)
    gate_up_sq = lax.psum(
        jnp.stack([jnp.sum(grad_gate * grad_gate, axis=1), jnp.sum(grad_up * grad_up, axis=1)]),
        "tp",
    )
    return (grad_tokens, grad_gain, grad_gate, grad_up, grad_down, gate_up_sq, down_sq)


def solution(mesh):
    placed = (
        P(("rep", "fs"), "tp"),
        P(),
        P("fs", "tp"),
        P("fs", "tp"),
        P("tp", "fs"),
        P(("rep", "fs"), "tp"),
    )
    return jax.shard_map(
        on_device,
        mesh=mesh,
        in_specs=placed,
        out_specs=(
            P(("rep", "fs"), "tp"),
            P("tp"),
            P("fs", "tp"),
            P("fs", "tp"),
            P("tp", "fs"),
            P(None, "fs"),
            P("tp"),
        ),
        check_vma=False,
    )
```
